256 devices in a mesh: sp: 64 (over z, y, core), tp: 4 (over x).
Axes of the slice: x: 4, y: 4, z: 8, core: 2. Of those that a mesh axis runs over, the one named last changes fastest.
Arguments:
- query_first: bfloat16 [16384, 512], P('sp', 'tp'), may hold values from -6 to 6
- key_first: bfloat16 [16384, 512], P('sp', 'tp'), may hold values from -6 to 6
- value_first: bfloat16 [16384, 1024], P('sp', 'tp'), may hold values from -6 to 6
- decay_first: float32 [16384, 512], P('sp', 'tp'), may hold values from -1 to 0
- gate_first: bfloat16 [16384, 1024], P('sp', 'tp'), may hold values from -6 to 6
- norm_first: float32 [256], replicated, may hold values from 0.1 to 1.9
- proj_first: bfloat16 [1024, 2048], P('tp', 'sp'), may hold values from -0.125 to 0.125
- query_second: bfloat16 [16384, 512], P('sp', 'tp'), may hold values from -6 to 6
- key_second: bfloat16 [16384, 512], P('sp', 'tp'), may hold values from -6 to 6
- value_second: bfloat16 [16384, 1024], P('sp', 'tp'), may hold values from -6 to 6
- decay_second: float32 [16384, 512], P('sp', 'tp'), may hold values from -1 to 0
- gate_second: bfloat16 [16384, 1024], P('sp', 'tp'), may hold values from -6 to 6
- norm_second: float32 [128], replicated, may hold values from 0.1 to 1.9
- proj_second: bfloat16 [1024, 2048], P('tp', 'sp'), may hold values from -0.125 to 0.125
- residual_in: bfloat16 [16384, 2048], P(('sp', 'tp')), may hold values from -6 to 6
- expert_norm: float32 [2048], replicated, may hold values from 0.1 to 1.9
- route_ids: int32 [16384, 2], P('sp'), may hold values from 0 to 63, all different within a row; in each aligned block of 256 rows (0 to 255, 256 to 511, ...) at most 16 rows name the same one
- route_weight: float32 [16384, 2], P('sp'), may hold values from 0.1 to 0.9
- expert_gate: bfloat16 [64, 2048, 3584], P('sp', None, 'tp'), may hold values from -0.125 to 0.125
- expert_up: bfloat16 [64, 2048, 3584], P('sp', None, 'tp'), may hold values from -0.125 to 0.125
- expert_down: bfloat16 [64, 3584, 2048], P('sp', 'tp'), may hold values from -0.09375 to 0.09375
Outputs:
- layer_out: bfloat16 [16384, 2048], P(('sp', 'tp'))
The draws below stay inside these ranges and needn't reach their ends.
Inputs may be any that keep to these rules, and one draw needn't show every extreme that they name: `route_ids`: each row names 2 different experts. Among the 256 rows of one index of sp no expert is named by more than 16 rows, and in every draw some expert is named by exactly 16 of them.
All inputs are finite; a program needn't handle non-finite values.
Results may differ from the reference program's by a relative error of at most 0.015.
Values may be sent and summed in bfloat16 or wider, within the bound.
No kernel may reach another device: no remote copies, remote signals or barrier semaphores. Data moves between devices by JAX's collectives and lax.ppermute only.
A program may use at most 64 MiB of HBM per device.

```python
import math
import jax
import jax.numpy as jnp
import numpy as np
from jax import lax

D = 2048
FF = 3584
HEADS_A = 4
KA = 128
VA = 256
HEADS_B = 8
KB = 64
VB = 128
TOPK = 2
BLK = 64
TOK_DEV = 256
TOKENS = 16384
EXPERTS = 64
CAP = 16
N_TP = 4


def decay_draw(key, count_of_tokens, feature_channels):
    random_subkeys = jax.random.split(key, 7)
    slow_share = 0.5
    gradual_mask = jax.random.uniform(random_subkeys[0], (feature_channels,), jnp.float32) < slow_share
    fast_rates = jnp.exp(jax.random.uniform(random_subkeys[1], (feature_channels,), jnp.float32, jnp.log(1.0 / 60.0), jnp.log(1.0 / 30.0)))
    slow_rates = jnp.exp(jax.random.uniform(random_subkeys[2], (feature_channels,), jnp.float32, jnp.log(0.05 / count_of_tokens), jnp.log(0.3 / count_of_tokens)))
    rates = jnp.where(gradual_mask, slow_rates, fast_rates)
    shard_factor = jnp.exp(jax.random.uniform(random_subkeys[3], (count_of_tokens // TOK_DEV,), jnp.float32, jnp.log(0.5), jnp.log(2.0)))
    shard_factor = jnp.repeat(shard_factor, TOK_DEV)
    roughness = jnp.exp(0.5 * jnp.clip(jax.random.normal(random_subkeys[4], (count_of_tokens, feature_channels), jnp.float32), -2.5, 2.5))
    decay_factors = -rates[None, :] * shard_factor[:, None] * roughness
    spike_position = jax.random.randint(random_subkeys[5], (3,), 0, count_of_tokens)
    spike_found = jnp.any(jnp.arange(count_of_tokens)[:, None] == spike_position[None, :], axis=1)
    spike_penalty = jnp.log(jax.random.uniform(random_subkeys[6], (feature_channels,), jnp.float32, 0.6, 0.8))
    decay_factors = decay_factors + jnp.where(spike_found[:, None] & gradual_mask[None, :], spike_penalty[None, :], 0.0)
    return decay_factors.astype(jnp.float32)


def draw_decay_first(key, part):
    return decay_draw(jax.random.fold_in(key, 11), TOKENS, HEADS_A * KA)


def draw_decay_second(key, part):
    return decay_draw(jax.random.fold_in(key, 23), TOKENS, HEADS_B * KB)


def block_levels(stream_key, extent, shards, low, top_value):
    def one(axis_at, parts):
        draws = jax.random.uniform(jax.random.fold_in(jax.random.fold_in(stream_key, 6), axis_at), (parts,), jnp.float32, low / len(shards), top_value / len(shards))
        return jnp.repeat(jnp.exp(draws), extent[axis_at] // parts).reshape((-1,) + (1,) * (len(extent) - axis_at - 1))

    factor_of = one(*shards[0])
    for cut in shards[1:]:
        factor_of = factor_of * one(*cut)
    return factor_of


def routed_block(rng, own, number, rows, amount, top, most, skew):
    order = jax.random.permutation(rng, amount)
    packed, ordinary = load_shares(amount, rows * top, most, skew, True), load_shares(amount, rows * top, most, skew, False)
    places = jnp.arange(amount)

    def named(sizes, offset_by):
        used = int((sizes > 0).sum())
        fixed = max(1, used // 4)
        shifted = fixed + (places - fixed + offset_by * (used - fixed)) % max(1, amount - fixed)
        return jnp.zeros((amount,), jnp.int32).at[order[jnp.where(places < fixed, places, shifted)]].set(jnp.asarray(sizes, jnp.int32))

    sizes = jnp.where(number % 4 == 0, named(packed, number // 4), named(ordinary, number - number // 4 - 1))
    mixed = jax.random.permutation(jax.random.fold_in(own, 3), amount)
    giver, receiver = mixed[0:amount // 2 * 2:2], mixed[1:amount // 2 * 2:2]
    slack = jnp.minimum(sizes[giver] - 1, most - sizes[receiver]) // 2
    slack = jnp.where((giver == order[0]) | (receiver == order[0]) | (sizes[receiver] == 0), 0, jnp.maximum(slack, 0))
    shifted = jax.random.randint(jax.random.fold_in(own, 4), (amount // 2,), 0, 1 << 20) % (slack + 1)
    sizes = sizes.at[giver].add(-shifted).at[receiver].add(shifted)
    labels = jnp.searchsorted(jnp.cumsum(sizes), jnp.arange(rows * top), side="right").astype(jnp.int32)
    grid = labels.reshape(top, rows).T
    grid = grid[jax.random.permutation(jax.random.fold_in(own, 1), rows)]
    offset_by = jax.random.randint(jax.random.fold_in(own, 2), (rows, 1), 0, top)
    return jnp.take_along_axis(grid, (jnp.arange(top)[None, :] + offset_by) % top, axis=1)


def load_shares(amount, total, most, skew, full):
    portions = [(1 << 20) // math.isqrt(grade ** skew) + 1 for grade in range(1, amount + 1)]
    largest = most if full else min(most, max(-(-total // amount), total * portions[0] // sum(portions)))
    least = 1 if total - largest >= amount - 1 else 0
    holding, surplus = [largest] + [least] * (amount - 1), total - largest - least * (amount - 1)
    while surplus > 0:
        candidates = [i for i in range(1, amount) if holding[i] < largest] or [i for i in range(1, amount) if holding[i] < most]
        mass, remaining = sum([portions[i] for i in candidates]), surplus
        for i in candidates:
            more = min(most - holding[i], max(1, remaining * portions[i] // mass), surplus)
            holding[i] = holding[i] + more
            surplus = surplus - more
    return np.array(holding)


def scatter_about(own_key, shape, deviation, reach, shards=(), held_as=jnp.bfloat16):
    gain = block_levels(own_key, shape, shards, -0.22, 0.18) if shards else 1.0
    entries = jax.random.normal(own_key, shape, jnp.float32) * deviation * gain
    return jnp.minimum(jnp.maximum(entries, -reach), reach).astype(held_as)


def setup_inputs(seed: int = 0) -> dict:
    arg_keys = jax.random.split(jax.random.key(seed), 22)
    query_first = scatter_about(arg_keys[0], (TOKENS, HEADS_A * KA), 1.0, 6.0, ((0, 64), (1, 4)))
    key_first = scatter_about(arg_keys[1], (TOKENS, HEADS_A * KA), 1.0, 6.0, ((0, 64), (1, 4)))
    value_first = scatter_about(arg_keys[2], (TOKENS, HEADS_A * VA), 1.0, 6.0, ((0, 64), (1, 4)))
    decay_first = draw_decay_first(jax.random.fold_in(arg_keys[21], 71), 0)
    gate_first = scatter_about(arg_keys[4], (TOKENS, HEADS_A * VA), 1.0, 6.0, ((0, 64), (1, 4)))
    norm_first = jnp.clip(1.0 + 0.18 * jax.random.normal(arg_keys[5], (VA,), jnp.float32), 0.1, 1.9)
    proj_first = scatter_about(arg_keys[6], (HEADS_A * VA, D), (HEADS_A * VA + HEADS_B * VB) ** -0.5, 0.125, ((0, 4), (1, 64)))
    query_second = scatter_about(arg_keys[7], (TOKENS, HEADS_B * KB), 1.0, 6.0, ((0, 64), (1, 4)))
    key_second = scatter_about(arg_keys[8], (TOKENS, HEADS_B * KB), 1.0, 6.0, ((0, 64), (1, 4)))
    value_second = scatter_about(arg_keys[9], (TOKENS, HEADS_B * VB), 1.0, 6.0, ((0, 64), (1, 4)))
    decay_second = draw_decay_second(jax.random.fold_in(arg_keys[21], 71), 0)
    gate_second = scatter_about(arg_keys[11], (TOKENS, HEADS_B * VB), 1.0, 6.0, ((0, 64), (1, 4)))
    norm_second = jnp.clip(1.0 + 0.18 * jax.random.normal(arg_keys[12], (VB,), jnp.float32), 0.1, 1.9)
    proj_second = scatter_about(arg_keys[13], (HEADS_B * VB, D), (HEADS_A * VA + HEADS_B * VB) ** -0.5, 0.125, ((0, 4), (1, 64)))
    residual_in = scatter_about(arg_keys[14], (TOKENS, D), 1.0, 6.0, ((0, 256),))
    expert_norm = jnp.clip(1.0 + 0.18 * jax.random.normal(arg_keys[15], (D,), jnp.float32), 0.1, 1.9)
    route_ids_keys = jax.random.split(jax.random.fold_in(arg_keys[16], 1), TOKENS // TOK_DEV)
    route_ids_turns = jax.random.permutation(jax.random.fold_in(arg_keys[16], 3), TOKENS // TOK_DEV)
    route_ids = jax.vmap(lambda own, number: routed_block(jax.random.fold_in(arg_keys[16], 2), own, number, TOK_DEV, EXPERTS, TOPK, CAP, 1))(route_ids_keys, route_ids_turns).reshape((TOKENS, TOPK))
    route_weight = jnp.clip(0.1 + 0.79999997 * jax.random.uniform(arg_keys[17], (TOKENS, TOPK), jnp.float32) ** block_levels(arg_keys[17], (TOKENS, TOPK), ((0, 64),), -0.2, 0.2), 0.1, 0.9)
    expert_gate = scatter_about(arg_keys[18], (EXPERTS, D, FF), D ** -0.5, 0.125, ((0, 64), (2, 4)))
    expert_up = scatter_about(arg_keys[19], (EXPERTS, D, FF), D ** -0.5, 0.125, ((0, 64), (2, 4)))
    expert_down = scatter_about(arg_keys[20], (EXPERTS, FF, D), FF ** -0.5, 0.09375, ((0, 64), (1, 4)))
    return dict(query_first=query_first, key_first=key_first, value_first=value_first, decay_first=decay_first, gate_first=gate_first, norm_first=norm_first, proj_first=proj_first, query_second=query_second, key_second=key_second, value_second=value_second, decay_second=decay_second, gate_second=gate_second, norm_second=norm_second, proj_second=proj_second, residual_in=residual_in, expert_norm=expert_norm, route_ids=route_ids, route_weight=route_weight, expert_gate=expert_gate, expert_up=expert_up, expert_down=expert_down)


epsilon = 1e-06
highest = lax.Precision.HIGHEST

def attend(queries, key_rows, values, decay_factors, key_width, value_width):
    count_of_tokens = queries.shape[0]
    head_count = queries.shape[1] // key_width
    blocks = count_of_tokens // BLK

    def arrange(source, feature_channels):
        return source.astype(jnp.float32).reshape(blocks, BLK, head_count, feature_channels).transpose(0, 2, 1, 3)
    causal = jnp.tril(jnp.ones((BLK, BLK), jnp.float32))

    def block_step(carry_state, inputs):
        query_block, key_block, value_block, decay_block = inputs
        cumulative = jnp.cumsum(decay_block, axis=1)
        block_end = cumulative[:, -1:, :]
        query_decayed = query_block * jnp.exp(cumulative)
        key_inverse = key_block * jnp.exp(-cumulative)
        key_to_end = key_block * jnp.exp(block_end - cumulative)
        scores = jnp.einsum('htd,hsd->hts', query_decayed, key_inverse, precision=highest) * causal
        outputs = jnp.einsum('hts,hsv->htv', scores, value_block, precision=highest)
        outputs = outputs + jnp.einsum('htd,hdv->htv', query_decayed, carry_state, precision=highest)
        carry_state = jnp.exp(block_end)[:, 0, :, None] * carry_state + jnp.einsum('hsd,hsv->hdv', key_to_end, value_block, precision=highest)
        return (carry_state, outputs)
    start_state = jnp.zeros((head_count, key_width, value_width), jnp.float32)
    scaled = arrange(queries, key_width) * key_width ** (-0.5)
    end_state, outputs = lax.scan(block_step, start_state, (scaled, arrange(key_rows, key_width), arrange(values, value_width), arrange(decay_factors, key_width)))
    return outputs.transpose(0, 2, 1, 3).reshape(count_of_tokens, head_count, value_width)

def head_norm(attention, head_gain, gate):
    inverse_rms = lax.rsqrt(lax.optimization_barrier(jnp.mean(attention * attention, axis=-1, keepdims=True)) + epsilon)
    gate_silu = jax.nn.silu(gate.astype(jnp.float32).reshape(attention.shape))
    mixed_rows = attention * inverse_rms * head_gain.astype(jnp.float32) * gate_silu
    return mixed_rows.astype(jnp.bfloat16).reshape(attention.shape[0], -1)

def route_tables(block_routes):
    flattened = block_routes.reshape(-1)
    onehot = (flattened[:, None] == jnp.arange(EXPERTS, dtype=jnp.int32)[None, :]).astype(jnp.int32)
    before = (jnp.cumsum(onehot, axis=0) - onehot).astype(jnp.int32)
    ranking = lax.optimization_barrier(jnp.sum(before * onehot, axis=1)).astype(jnp.int32)
    slot_ids = (flattened * CAP + ranking).astype(jnp.int32)
    row_token = (jnp.arange(TOK_DEV * TOPK, dtype=jnp.int32) // TOPK).astype(jnp.int32)
    owners = jnp.full((EXPERTS * CAP,), TOK_DEV, jnp.int32).at[slot_ids].set(row_token)
    return (owners, slot_ids)

def place_weights(slot_ids, weights):
    return jnp.zeros((EXPERTS * CAP,), jnp.float32).at[slot_ids].set(weights.astype(jnp.float32))

def pick_rows(block_rows, index_list):
    return jnp.take(block_rows, index_list, axis=0)

def reference(query_first, key_first, value_first, decay_first, gate_first, norm_first, proj_first, query_second, key_second, value_second, decay_second, gate_second, norm_second, proj_second, residual_in, expert_norm, route_ids, route_weight, expert_gate, expert_up, expert_down):
    attention_first = attend(query_first, key_first, value_first, decay_first, KA, VA)
    attention_second = attend(query_second, key_second, value_second, decay_second, KB, VB)
    mixed_first = head_norm(attention_first, norm_first, gate_first)
    mixed_second = head_norm(attention_second, norm_second, gate_second)
    rows_first = HEADS_A // N_TP * VA
    rows_second = HEADS_B // N_TP * VB
    mixture = jnp.zeros((TOKENS, D), jnp.float32)
    for portion in range(N_TP):
        portion_sum = jnp.dot(mixed_first[:, portion * rows_first:(portion + 1) * rows_first], proj_first[portion * rows_first:(portion + 1) * rows_first], preferred_element_type=jnp.float32)
        portion_sum = portion_sum + jnp.dot(mixed_second[:, portion * rows_second:(portion + 1) * rows_second], proj_second[portion * rows_second:(portion + 1) * rows_second], preferred_element_type=jnp.float32)
        rounded = lax.optimization_barrier(portion_sum.astype(jnp.bfloat16))
        mixture = mixture + rounded.astype(jnp.float32)
    residual = (residual_in.astype(jnp.float32) + mixture).astype(jnp.bfloat16)
    as_float = residual.astype(jnp.float32)
    inverse_rms = lax.rsqrt(lax.optimization_barrier(jnp.mean(as_float * as_float, axis=-1, keepdims=True)) + epsilon)
    normed = (as_float * inverse_rms * expert_norm.astype(jnp.float32)).astype(jnp.bfloat16)
    block_count = TOKENS // TOK_DEV
    owners, slot_ids = jax.vmap(route_tables)(route_ids.reshape(block_count, TOK_DEV, TOPK))
    slot_weight = jax.vmap(place_weights)(slot_ids, route_weight.reshape(block_count, TOK_DEV * TOPK))
    padded = jnp.concatenate((normed.reshape(block_count, TOK_DEV, D), jnp.zeros((block_count, 1, D), jnp.bfloat16)), axis=1)
    block_base = (jnp.arange(block_count, dtype=jnp.int32) * TOK_DEV).astype(jnp.int32)[:, None]
    quarter_width = FF // N_TP

    def expert_step(combined, inputs):
        gate_matrix, up_matrix, down_matrix, expert = inputs
        chosen = lax.dynamic_slice_in_dim(owners, (expert * CAP).astype(jnp.int32), CAP, 1)
        gathered = jax.vmap(pick_rows)(padded, chosen)
        flattened = gathered.reshape(block_count * CAP, D)
        gate_part = jnp.dot(flattened, gate_matrix, preferred_element_type=jnp.float32)
        up_part = jnp.dot(flattened, up_matrix, preferred_element_type=jnp.float32)
        hidden = (jax.nn.silu(gate_part) * up_part).astype(jnp.bfloat16)
        summed = jnp.zeros((block_count * CAP, D), jnp.float32)
        for portion in range(N_TP):
            piece = jnp.dot(hidden[:, portion * quarter_width:(portion + 1) * quarter_width], down_matrix[portion * quarter_width:(portion + 1) * quarter_width], preferred_element_type=jnp.float32)
            rounded = lax.optimization_barrier(piece.astype(jnp.bfloat16))
            summed = summed + rounded.astype(jnp.float32)
        weights_here = lax.dynamic_slice_in_dim(slot_weight, (expert * CAP).astype(jnp.int32), CAP, 1).reshape(-1, 1)
        targets = jnp.where(chosen == TOK_DEV, TOKENS, block_base + chosen).astype(jnp.int32).reshape(-1)
        combined = combined.at[targets].add(summed * weights_here)
        return (combined, None)
    combined_start = jnp.zeros((TOKENS + 1, D), jnp.float32)
    combined, _ = lax.scan(expert_step, combined_start, (expert_gate, expert_up, expert_down, jnp.arange(EXPERTS, dtype=jnp.int32)))
    return (residual.astype(jnp.float32) + combined[:TOKENS]).astype(jnp.bfloat16)
```

```python
import jax
import jax.numpy as jnp
from jax import lax
from jax.experimental import pallas as pl
from jax.sharding import Mesh
from jax.sharding import PartitionSpec as P


KA = 128
VA = 256
KB = 64
VB = 128
BLK = 64
CHUNKS = 2
SP = ("sp_0", "sp_1", "sp_2")
SP_TP = ("sp_0", "sp_1", "sp_2", "tp")


epsilon = 1e-06
highest = lax.Precision.HIGHEST


def exact_dot(left, right, contract=(1, 0)):
    return lax.dot_general(
        left.astype(jnp.float32),
        right.astype(jnp.float32),
        (((contract[0],), (contract[1],)), ((), ())),
        precision=highest,
        preferred_element_type=jnp.float32,
    )


def grid_of(shape, dim):
    return lax.broadcasted_iota(jnp.int32, shape, dim)


def of_head(value, head, width):
    inside = grid_of(value.shape, 1) // width == head
    return jnp.where(inside, value, 0.0)


def call(kernel, outs, *operands, flops=10_000_000):
    moved = sum(x.size * x.dtype.itemsize for x in (*operands, *outs))
    return pl.pallas_call(
        kernel,
        out_shape=[jax.ShapeDtypeStruct(x.shape, x.dtype) for x in outs],
        cost_estimate=pl.CostEstimate(flops=flops, bytes_accessed=moved, transcendentals=0),
    )(*operands)


def shaped(shape, dtype):
    return jax.ShapeDtypeStruct(shape, dtype)


def three_parts(value):
    coarse = value.astype(jnp.bfloat16).astype(jnp.float32)
    middle = (value - coarse).astype(jnp.bfloat16).astype(jnp.float32)
    return coarse, middle, value - coarse - middle


def state_kernel(key_a, value_a, decay_a, key_b, value_b, decay_b, out_ref):
    tokens, width = key_a.shape
    later = (grid_of((tokens, tokens), 1) > grid_of((tokens, tokens), 0)).astype(jnp.float32)
    every = jnp.ones((tokens, width), jnp.float32)

    def to_end(key_rows, decay):
        return key_rows[...].astype(jnp.float32) * jnp.exp(exact_dot(later, decay[...]))

    ended_a, ended_b = to_end(key_a, decay_a), to_end(key_b, decay_b)
    out_ref[:, :VA] = exact_dot(ended_a.T, value_a[...]).astype(jnp.bfloat16)
    state_b = exact_dot(of_head(ended_b, 0, KB).T, value_b[:, :VB])
    state_b = state_b + exact_dot(of_head(ended_b, 1, KB).T, value_b[:, VB:])
    out_ref[:, VA : VA + VB] = state_b.astype(jnp.bfloat16)
    lane = grid_of((width, width), 1)
    totals = jnp.zeros((width, width), jnp.float32)
    for first, decay in ((0, decay_a), (3, decay_b)):
        for k, part in enumerate(three_parts(exact_dot(decay[...].T, every))):
            totals = jnp.where(lane == first + k, part, totals)
    out_ref[:, VA + VB :] = totals.astype(jnp.bfloat16)


def totals_of(block):
    lanes = block[:, VA + VB :].astype(jnp.float32)
    lane = grid_of(lanes.shape, 1)
    total_a = jnp.sum(jnp.where(lane < 3, lanes, 0.0), axis=1, keepdims=True)
    total_b = jnp.sum(jnp.where((lane >= 3) & (lane < 6), lanes, 0.0), axis=1, keepdims=True)
    return total_a, total_b


def wide(total_a, total_b):
    rows = total_a.shape[0]
    return jnp.concatenate(
        (jnp.broadcast_to(total_a, (rows, VA)), jnp.broadcast_to(total_b, (rows, VB))), axis=1
    )


def plane_kernel(in_ref, send_ref, prefix_ref, passed_ref):
    members, rows, _ = in_ref.shape
    running = jnp.zeros((rows, VA + VB), jnp.float32)
    passed_a = passed_b = jnp.zeros((rows, 1), jnp.float32)
    for k in range(members):
        prefix_ref[k] = running
        passed_ref[k] = wide(passed_a, passed_b)
        block = in_ref[k]
        total_a, total_b = totals_of(block)
        decayed = running * jnp.exp(wide(total_a, total_b))
        running = decayed + block[:, : VA + VB].astype(jnp.float32)
        passed_a, passed_b = passed_a + total_a, passed_b + total_b
    send_ref[:, : VA + VB] = running.astype(jnp.bfloat16)
    lane = grid_of((rows, 128), 1)
    totals = jnp.zeros((rows, 128), jnp.float32)
    for first, total in ((0, passed_a), (3, passed_b)):
        for k, part in enumerate(three_parts(jnp.broadcast_to(total, (rows, 128)))):
            totals = jnp.where(lane == first + k, part, totals)
    send_ref[:, VA + VB :] = totals.astype(jnp.bfloat16)


def entering_kernel(planes, prefix_ref, passed_ref, out_ref):
    members, rows, _ = prefix_ref.shape
    before = jnp.zeros((rows, VA + VB), jnp.float32)
    for k in range(planes.shape[0]):
        block = planes[k]
        before = before * jnp.exp(wide(*totals_of(block)))
        before = before + block[:, : VA + VB].astype(jnp.float32)
    for k in range(members):
        out_ref[k] = (jnp.exp(passed_ref[k]) * before + prefix_ref[k]).astype(jnp.bfloat16)


def local_kernel(
    query_a, key_a, value_a, decay_a, query_b, key_b, value_b, decay_b, out_a, read_a, out_b, read_b
):
    tokens, width = key_a.shape
    row, column = grid_of((tokens, tokens), 0), grid_of((tokens, tokens), 1)
    upto = (column <= row).astype(jnp.float32)
    within = ((column <= row) & (column // BLK == row // BLK)).astype(jnp.float32)
    causal = grid_of((BLK, BLK), 1) <= grid_of((BLK, BLK), 0)
    every = jnp.ones((BLK, width), jnp.float32)
    groups = (
        (query_a, key_a, value_a, decay_a, out_a, read_a, KA, VA),
        (query_b, key_b, value_b, decay_b, out_b, read_b, KB, VB),
    )
    for query, key_rows, value, decay, out, read, key_width, value_width in groups:
        heads = width // key_width
        scaled = query[...].astype(jnp.float32) * key_width ** (-0.5)
        read[...] = scaled * jnp.exp(exact_dot(upto, decay[...]))
        cumulative = exact_dot(within, decay[...])
        decayed = scaled * jnp.exp(cumulative)
        plain_keys = key_rows[...].astype(jnp.float32)
        inverse = plain_keys * jnp.exp(-cumulative)
        states = [jnp.zeros((width, value_width), jnp.float32)] * heads
        for at in range(0, tokens, BLK):
            block = slice(at, at + BLK)
            end = cumulative[at + BLK - 1 : at + BLK]
            to_end = plain_keys[block] * jnp.exp(end - cumulative[block])
            kept = jnp.exp(exact_dot(decay[block].T, every))
            if value_width > width:
                kept = jnp.concatenate([kept] * (value_width // width), axis=1)
            for h in range(heads):
                lanes = slice(h * value_width, (h + 1) * value_width)
                values = value[block, lanes].astype(jnp.float32)
                reading = of_head(decayed[block], h, key_width)
                scores = jnp.where(causal, exact_dot(reading, inverse[block].T), 0.0)
                result = exact_dot(scores, values)
                if at:
                    result = result + exact_dot(reading, states[h])
                out[block, lanes] = result
                if at + BLK < tokens:
                    added = exact_dot(of_head(to_end, h, key_width).T, values)
                    states[h] = kept * states[h] + added


def mix_kernel(
    local_a, read_a, local_b, read_b, state, gate_a, gate_b, norm_a, norm_b, weights, out_ref
):
    state_a, state_b = state[:, :VA], state[:, VA : VA + VB]

    def mixed(attention, gain, gate):
        mean = jnp.mean(attention * attention, axis=-1, keepdims=True)
        rows = attention * lax.rsqrt(mean + epsilon) * gain[...]
        return (rows * jax.nn.silu(gate.astype(jnp.float32))).astype(jnp.bfloat16)

    parts = [mixed(local_a[...] + exact_dot(read_a[...], state_a), norm_a, gate_a[...])]
    for h in range(2):
        lanes = slice(h * VB, (h + 1) * VB)
        attention = local_b[:, lanes] + exact_dot(of_head(read_b[...], h, KB), state_b)
        parts.append(mixed(attention, norm_b, gate_b[:, lanes]))
    rows = jnp.concatenate(parts, axis=1)
    width = out_ref.shape[2]
    for k in range(out_ref.shape[0]):
        out_ref[k] = lax.dot_general(
            rows,
            weights[k * width : (k + 1) * width],
            (((1,), (1,)), ((), ())),
            preferred_element_type=jnp.float32,
        ).astype(jnp.bfloat16)


def moved(value, axis, step):
    size = lax.axis_size(axis)
    return lax.ppermute(value, axis, [(k, (k + step) % size) for k in range(size)])


def placed(own, axis, values_by_step):
    size, me = lax.axis_size(axis), lax.axis_index(axis)
    whole = jnp.zeros((size, *own.shape), own.dtype)
    for step, value in ((0, own), *values_by_step):
        whole = lax.dynamic_update_index_in_dim(whole, value, (me - step) % size, 0)
    return whole


def doubled(value, axis, partner_of, first):
    pairs = [(k, partner_of(k)) for k in range(lax.axis_size(axis))]
    other = lax.ppermute(value, axis, pairs)
    return jnp.stack((jnp.where(first, value, other), jnp.where(first, other, value)), axis=0)


def whole_projection(own):
    z, y, core = (lax.axis_index(name) for name in SP)
    rows, width = own.shape
    value = doubled(own, SP[0], lambda k: k ^ 1, z % 2 == 0)
    value = doubled(value, SP[0], lambda k: k ^ 2, z // 2 % 2 == 0)
    value = doubled(value, SP[0], lambda k: k ^ 4, z // 4 == 0)
    value = value.reshape(-1, rows, width)
    value = doubled(value, SP[1], lambda k: k ^ 1, y % 2 == 0)
    value = doubled(value, SP[1], lambda k: 3 - k, y // 2 == 0)
    value = value.reshape(-1, *value.shape[2:])
    value = doubled(value, SP[2], lambda k: k ^ 1, core == 0)
    return jnp.transpose(value, (2, 1, 0, 3, 4)).reshape(-1, width)


def exchanged_by_steps(value, axis, dim):
    size, me = lax.axis_size(axis), lax.axis_index(axis)
    width = value.shape[dim] // size

    def piece(at):
        return lax.dynamic_slice_in_dim(value, at * width, width, axis=dim)

    steps = range(1, size)
    return placed(
        piece(me), axis, [(step, moved(piece((me + step) % size), axis, step)) for step in steps]
    )


def rms_scale(residual, gain_vector):
    as_float = residual.astype(jnp.float32)
    inverse_rms = lax.rsqrt(jnp.mean(as_float * as_float, axis=-1, keepdims=True) + epsilon)
    return (as_float * inverse_rms * gain_vector).astype(jnp.bfloat16)


def one_hot_slots(block_routes, experts, capacity):
    tokens, top_count = block_routes.shape
    pairs = tokens * top_count
    named = block_routes.reshape(-1, 1) == jnp.arange(experts, dtype=jnp.int32)[None, :]
    named = named.astype(jnp.bfloat16)
    earlier = jnp.tril(jnp.ones((pairs, pairs), jnp.bfloat16), -1)
    before = jnp.dot(earlier, named, preferred_element_type=jnp.float32)
    ranking = jnp.sum(before * named.astype(jnp.float32), axis=1).astype(jnp.int32)
    return (block_routes.reshape(-1) * capacity + ranking).reshape(tokens, top_count)


def ring_gather(own, axis):
    half = own.shape[0] // 2
    before, after = moved(own, axis, 1), moved(own, axis, -1)
    upper, lower = moved(before[:half], axis, 1), moved(after[half:], axis, -1)
    return before, after, jnp.concatenate((upper, lower), axis=0)


def ring_sum(block_of, axis):
    size, me = lax.axis_size(axis), lax.axis_index(axis)
    far = block_of((me + 2) % size)
    half = far.shape[0] // 2
    upper, lower = moved(far[:half], axis, 1), moved(far[half:], axis, -1)
    right = block_of((me + 1) % size).astype(jnp.float32)
    left = block_of((me + size - 1) % size).astype(jnp.float32)
    right = jnp.concatenate((right[:half] + upper.astype(jnp.float32), right[half:]), axis=0)
    left = jnp.concatenate((left[:half], left[half:] + lower.astype(jnp.float32)), axis=0)
    from_left = moved(right.astype(jnp.bfloat16), axis, 1)
    from_right = moved(left.astype(jnp.bfloat16), axis, -1)
    own = block_of(me).astype(jnp.float32)
    return own + from_left.astype(jnp.float32) + from_right.astype(jnp.float32)


def layer(
    query_first,
    key_first,
    value_first,
    decay_first,
    gate_first,
    norm_first,
    proj_first,
    query_second,
    key_second,
    value_second,
    decay_second,
    gate_second,
    norm_second,
    proj_second,
    residual_in,
    expert_norm,
    route_ids,
    route_weight,
    expert_gate,
    expert_up,
    expert_down,
):
    bf16, f32 = jnp.bfloat16, jnp.float32
    tokens = query_first.shape[0]
    projection = whole_projection(jnp.concatenate((proj_first, proj_second), axis=0).T)
    tp_size = lax.axis_size("tp")
    columns = residual_in.reshape(residual_in.shape[0], tp_size, -1).swapaxes(0, 1)
    residual_part = lax.all_to_all(columns, "tp", 0, 0, tiled=True).reshape(tokens, -1)
    plane_size = lax.axis_size(SP[1]) * lax.axis_size(SP[2])
    planes = lax.axis_size(SP[0])
    sent = VA + VB + 128
    (states,) = call(
        state_kernel,
        [shaped((KA, sent), bf16)],
        key_first,
        value_first,
        decay_first,
        key_second,
        value_second,
        decay_second,
    )
    in_plane = lax.all_to_all(
        states.reshape(plane_size, KA // plane_size, sent), SP[1:], 0, 0, tiled=True
    )
    local_first, read_first, local_second, read_second = call(
        local_kernel,
        [shaped((tokens, n), f32) for n in (VA, KA, 2 * VB, 2 * KB)],
        query_first,
        key_first,
        value_first,
        decay_first,
        query_second,
        key_second,
        value_second,
        decay_second,
        flops=2_000_000_000,
    )
    own_plane, prefix, passed = call(
        plane_kernel,
        [
            shaped(in_plane.shape[1:], bf16),
            shaped((*in_plane.shape[:2], VA + VB), f32),
            shaped((*in_plane.shape[:2], VA + VB), f32),
        ],
        in_plane,
    )
    later = jnp.arange(planes)[:, None, None] > lax.axis_index(SP[0])
    told = jnp.where(later, own_plane[None], jnp.zeros((), bf16))
    earlier = lax.all_to_all(told, SP[0], split_axis=0, concat_axis=0, tiled=True)
    (entering,) = call(
        entering_kernel, [shaped(prefix.shape, bf16)], earlier, prefix, passed
    )
    carried = lax.all_to_all(entering, SP[1:], 0, 0, tiled=True).reshape(KA, VA + VB)
    tp_index = lax.axis_index("tp")
    (partial_terms,) = call(
        mix_kernel,
        [shaped((tp_size, tokens, projection.shape[0] // tp_size), bf16)],
        local_first,
        read_first,
        local_second,
        read_second,
        carried,
        gate_first,
        gate_second,
        norm_first.reshape(1, VA),
        norm_second.reshape(1, VB),
        projection,
    )
    block_tokens, top_count = route_ids.shape
    experts = lax.axis_size(SP)
    capacity = 2 * top_count * block_tokens // experts
    arrived = lax.all_to_all(partial_terms, "tp", split_axis=0, concat_axis=0, tiled=True)
    mixture = arrived.astype(jnp.float32).sum(axis=0)
    residual = (residual_part.astype(jnp.float32) + mixture).astype(jnp.bfloat16)
    slots = one_hot_slots(route_ids, experts, capacity)
    width = residual.shape[1]
    model_width = width * tp_size
    share = capacity // CHUNKS
    rows_here = experts * share
    numbers = jnp.arange(rows_here, dtype=jnp.int32)
    waiting, shares = [], []
    for k in range(CHUNKS):
        held = numbers // share * capacity + k * share + numbers % share
        chosen = slots[:, :, None] == held[None, None, :]
        carries = jnp.any(chosen, axis=1).astype(bf16)
        shares.append(jnp.sum(jnp.where(chosen, route_weight[:, :, None], 0.0), axis=1))
        outgoing = lax.dot_general(
            carries, residual, (((0,), (0,)), ((), ())), preferred_element_type=f32
        ).astype(bf16)
        waiting.append(
            lax.all_to_all(outgoing.reshape(experts, share, width), SP, 0, 0, tiled=True)
        )
    returned = []
    for k in range(CHUNKS):
        incoming = waiting[k].reshape(rows_here, width)
        before, after, far = ring_gather(incoming, "tp")
        rows = jnp.zeros((rows_here, model_width), bf16)
        for part, step in ((incoming, 0), (before, tp_size - 1), (after, 1), (far, 2)):
            rows = lax.dynamic_update_slice_in_dim(
                rows, part, (tp_index + step) % tp_size * width, axis=1
            )
        normed = rms_scale(rows, expert_norm)
        gate_part = jnp.dot(normed, expert_gate[0], preferred_element_type=f32)
        up_part = jnp.dot(normed, expert_up[0], preferred_element_type=f32)
        hidden = (jax.nn.silu(gate_part) * up_part).astype(bf16)
        produced = jnp.dot(hidden, expert_down[0], preferred_element_type=f32).astype(bf16)
        summed = ring_sum(
            lambda at: lax.dynamic_slice_in_dim(produced, at * width, width, axis=1), "tp"
        ).astype(bf16)
        returned.append(lax.all_to_all(summed.reshape(experts, share, width), SP, 0, 0, tiled=True))
    combined = jnp.zeros((block_tokens, width), f32)
    for weights, back in zip(shares, returned):
        back = back.reshape(rows_here, width)
        coarse = lax.reduce_precision(weights, 8, 7)
        middle = lax.reduce_precision(weights - coarse, 8, 7)
        fine = weights - coarse - middle
        for portion in (coarse, middle, fine):
            combined = combined + jnp.dot(portion.astype(bf16), back, preferred_element_type=f32)
    layer_part = (residual.astype(jnp.float32) + combined).astype(jnp.bfloat16)
    whole = exchanged_by_steps(layer_part, "tp", 0)
    return jnp.moveaxis(whole, 0, 1).reshape(block_tokens // tp_size, model_width)


def solution(mesh):
    split = Mesh(mesh.devices.reshape(8, 4, 2, mesh.shape["tp"]), ("sp_0", "sp_1", "sp_2", "tp"))
    in_specs = (
        P(SP, "tp"),
        P(SP, "tp"),
        P(SP, "tp"),
        P(SP, "tp"),
        P(SP, "tp"),
        P(),
        P("tp", SP),
        P(SP, "tp"),
        P(SP, "tp"),
        P(SP, "tp"),
        P(SP, "tp"),
        P(SP, "tp"),
        P(),
        P("tp", SP),
        P(SP_TP, None),
        P(),
        P(SP, None),
        P(SP, None),
        P(SP, None, "tp"),
        P(SP, None, "tp"),
        P(SP, "tp", None),
    )
    out_specs = P(SP_TP, None)
    return jax.shard_map(layer, mesh=split, in_specs=in_specs, out_specs=out_specs, check_vma=False)
```

```python
import jax
import jax.numpy as jnp
from jax import lax
from jax.experimental import pallas as pl
from jax.experimental.pallas import tpu as pltpu
from jax.sharding import Mesh
from jax.sharding import PartitionSpec as P


KA = 128
VA = 256
KB = 64
VB = 128
BLK = 64
CHUNKS = 1
SP = ("sp_0", "sp_1", "sp_2")
SP_TP = ("sp_0", "sp_1", "sp_2", "tp")


epsilon = 1e-06


def plain_dot(left, right):
    return jnp.dot(left, right, preferred_element_type=jnp.float32)


def two_parts(value):
    coarse = value.astype(jnp.bfloat16)
    return coarse, (value - coarse.astype(jnp.float32)).astype(jnp.bfloat16)


def dot_given(left, right):
    coarse, fine = two_parts(left)
    right = right.astype(jnp.bfloat16)
    return plain_dot(coarse, right) + plain_dot(fine, right)


def dot_both(left, right):
    left, left_fine = two_parts(left)
    right, right_fine = two_parts(right)
    small = plain_dot(left, right_fine) + plain_dot(left_fine, right)
    return plain_dot(left, right) + small


def summed_where(mask, value):
    width = value.shape[1]
    parts = [part.astype(jnp.bfloat16) for part in three_parts(value)]
    sums = plain_dot(mask.astype(jnp.bfloat16), jnp.concatenate(parts, axis=1))
    return sums[:, :width] + sums[:, width : 2 * width] + sums[:, 2 * width :]


def column_sums(value):
    width = value.shape[1]
    turned = value.T
    parts = [part.astype(jnp.bfloat16) for part in three_parts(turned)]
    every = jnp.ones((value.shape[0], width), jnp.bfloat16)
    sums = plain_dot(jnp.concatenate(parts, axis=0), every)
    return sums[:width] + sums[width : 2 * width] + sums[2 * width :]


def grid_of(shape, dim):
    return lax.broadcasted_iota(jnp.int32, shape, dim)


def of_head(value, head, width):
    inside = grid_of(value.shape, 1) // width == head
    return jnp.where(inside, value, 0.0)


def call(kernel, outs, *operands, place=(), flops=10_000_000):
    moved_bytes = sum(x.size * x.dtype.itemsize for x in (*operands, *outs))
    inside = pl.BlockSpec(memory_space=pltpu.VMEM)
    scratch = [pltpu.VMEM((2048, 512), jnp.bfloat16)] if kernel is mix_kernel else []
    return pl.pallas_call(
        kernel,
        out_shape=[jax.ShapeDtypeStruct(x.shape, x.dtype) for x in outs],
        in_specs=[pl.BlockSpec(memory_space=pltpu.SMEM)] * len(place)
        + [inside] * len(operands),
        out_specs=[inside] * len(outs),
        scratch_shapes=scratch,
        cost_estimate=pl.CostEstimate(flops=flops, bytes_accessed=moved_bytes, transcendentals=0),
    )(*[jnp.stack(numbers).astype(jnp.int32) for numbers in place], *operands)


def shaped(shape, dtype):
    return jax.ShapeDtypeStruct(shape, dtype)


def three_parts(value):
    coarse = value.astype(jnp.bfloat16).astype(jnp.float32)
    middle = (value - coarse).astype(jnp.bfloat16).astype(jnp.float32)
    return coarse, middle, value - coarse - middle


def state_kernel(key_a, value_a, decay_a, key_b, value_b, decay_b, out_ref):
    tokens, width = key_a.shape
    later = (grid_of((tokens, tokens), 1) > grid_of((tokens, tokens), 0)).astype(jnp.float32)

    def to_end(key_rows, decay):
        return key_rows[...].astype(jnp.float32) * jnp.exp(summed_where(later, decay[...]))

    ended_a, ended_b = to_end(key_a, decay_a), to_end(key_b, decay_b)
    out_ref[:, :VA] = dot_given(ended_a.T, value_a[...]).astype(jnp.bfloat16)
    state_b = dot_given(of_head(ended_b, 0, KB).T, value_b[:, :VB])
    state_b = state_b + dot_given(of_head(ended_b, 1, KB).T, value_b[:, VB:])
    out_ref[:, VA : VA + VB] = state_b.astype(jnp.bfloat16)
    lane = grid_of((width, width), 1)
    totals = jnp.zeros((width, width), jnp.float32)
    for first, decay in ((0, decay_a), (3, decay_b)):
        for k, part in enumerate(three_parts(column_sums(decay[...]))):
            totals = jnp.where(lane == first + k, part, totals)
    out_ref[:, VA + VB :] = totals.astype(jnp.bfloat16)


def totals_of(block):
    lanes = block[:, VA + VB :].astype(jnp.float32)
    lane = grid_of(lanes.shape, 1)
    total_a = jnp.sum(jnp.where(lane < 3, lanes, 0.0), axis=1, keepdims=True)
    total_b = jnp.sum(jnp.where((lane >= 3) & (lane < 6), lanes, 0.0), axis=1, keepdims=True)
    return total_a, total_b


def wide(total_a, total_b):
    rows = total_a.shape[0]
    return jnp.concatenate(
        (jnp.broadcast_to(total_a, (rows, VA)), jnp.broadcast_to(total_b, (rows, VB))), axis=1
    )


def plane_kernel(place, in_ref, send_ref, prefix_ref, passed_ref):
    members, rows, _ = in_ref.shape
    running = jnp.zeros((rows, VA + VB), jnp.float32)
    passed_a = passed_b = jnp.zeros((rows, 1), jnp.float32)
    for k in range(members):
        prefix_ref[k] = running
        passed_ref[k] = wide(passed_a, passed_b)
        block = in_ref[k]
        total_a, total_b = totals_of(block)
        decayed = running * jnp.exp(wide(total_a, total_b))
        running = decayed + block[:, : VA + VB].astype(jnp.float32)
        passed_a, passed_b = passed_a + total_a, passed_b + total_b
    lane = grid_of((rows, 128), 1)
    totals = jnp.zeros((rows, 128), jnp.float32)
    for first, total in ((0, passed_a), (3, passed_b)):
        for k, part in enumerate(three_parts(jnp.broadcast_to(total, (rows, 128)))):
            totals = jnp.where(lane == first + k, part, totals)
    message = jnp.concatenate((running, totals), axis=1).astype(jnp.bfloat16)
    for k in range(send_ref.shape[0]):
        send_ref[k] = jnp.where(place[0] < k, message, jnp.zeros_like(message))


def entering_kernel(planes, prefix_ref, passed_ref, out_ref):
    members, rows, _ = prefix_ref.shape
    before = jnp.zeros((rows, VA + VB), jnp.float32)
    for k in range(planes.shape[0]):
        block = planes[k, :rows]
        before = before * jnp.exp(wide(*totals_of(block)))
        before = before + block[:, : VA + VB].astype(jnp.float32)
    for k in range(members):
        out_ref[k] = (jnp.exp(passed_ref[k]) * before + prefix_ref[k]).astype(jnp.bfloat16)


def local_kernel(
    query_a, key_a, value_a, decay_a, query_b, key_b, value_b, decay_b, out_a, read_a, out_b, read_b
):
    tokens, width = key_a.shape
    row, column = grid_of((tokens, tokens), 0), grid_of((tokens, tokens), 1)
    upto = (column <= row).astype(jnp.float32)
    within = ((column <= row) & (column // BLK == row // BLK)).astype(jnp.float32)
    causal = grid_of((BLK, BLK), 1) <= grid_of((BLK, BLK), 0)
    groups = (
        (query_a, key_a, value_a, decay_a, out_a, read_a, KA, VA),
        (query_b, key_b, value_b, decay_b, out_b, read_b, KB, VB),
    )
    for query, key_rows, value, decay, out, read, key_width, value_width in groups:
        heads = width // key_width
        scaled = query[...].astype(jnp.float32) * key_width ** (-0.5)
        read[...] = scaled * jnp.exp(summed_where(upto, decay[...]))
        cumulative = summed_where(within, decay[...])
        decayed = scaled * jnp.exp(cumulative)
        plain_keys = key_rows[...].astype(jnp.float32)
        inverse = plain_keys * jnp.exp(-cumulative)
        states = [jnp.zeros((width, value_width), jnp.float32)] * heads
        for at in range(0, tokens, BLK):
            block = slice(at, at + BLK)
            end = cumulative[at + BLK - 1 : at + BLK]
            to_end = plain_keys[block] * jnp.exp(end - cumulative[block])
            kept = jnp.exp(column_sums(decay[block]))
            if value_width > width:
                kept = jnp.concatenate([kept] * (value_width // width), axis=1)
            for h in range(heads):
                lanes = slice(h * value_width, (h + 1) * value_width)
                values = value[block, lanes]
                reading = of_head(decayed[block], h, key_width)
                scores = jnp.where(causal, dot_both(reading, inverse[block].T), 0.0)
                result = dot_given(scores, values)
                if at:
                    result = result + dot_both(reading, states[h])
                out[block, lanes] = result
                if at + BLK < tokens:
                    added = dot_given(of_head(to_end, h, key_width).T, values)
                    states[h] = kept * states[h] + added


def mix_kernel(
    place,
    local_a,
    read_a,
    local_b,
    read_b,
    state,
    gate_a,
    gate_b,
    norm_a,
    norm_b,
    mine,
    other,
    residual,
    out_ref,
    weights,
):
    sides, planes, height, _ = mine.shape
    for step in range(sides):
        y = lax.rem(place[0] + sides - (0, 1, 3, 2)[step], sides)
        for z in range(planes):
            for core, source in ((place[1], mine), (1 - place[1], other)):
                at = ((z * sides + y) * 2 + core) * height
                weights[pl.ds(pl.multiple_of(at, height), height), :] = source[step, z]
    state_a, state_b = state[:, :VA], state[:, VA : VA + VB]

    def mixed(attention, gain, gate):
        mean = jnp.mean(attention * attention, axis=-1, keepdims=True)
        rows = attention * lax.rsqrt(mean + epsilon) * gain[...]
        return (rows * jax.nn.silu(gate.astype(jnp.float32))).astype(jnp.bfloat16)

    parts = [mixed(local_a[...] + dot_given(read_a[...], state_a), norm_a, gate_a[...])]
    for h in range(2):
        lanes = slice(h * VB, (h + 1) * VB)
        attention = local_b[:, lanes] + dot_given(of_head(read_b[...], h, KB), state_b)
        parts.append(mixed(attention, norm_b, gate_b[:, lanes]))
    rows = jnp.concatenate(parts, axis=1)
    width = out_ref.shape[2]
    for k in range(out_ref.shape[0]):
        out_ref[k, : rows.shape[0]] = lax.dot_general(
            rows,
            weights[k * width : (k + 1) * width],
            (((1,), (1,)), ((), ())),
            preferred_element_type=jnp.float32,
        ).astype(jnp.bfloat16)
        out_ref[k, rows.shape[0] :] = residual[:, k * width : (k + 1) * width]


def moved(value, axis, step):
    size = lax.axis_size(axis)
    return lax.ppermute(value, axis, [(k, (k + step) % size) for k in range(size)])


def around(own, axis):
    half = own.shape[0] // 2
    before, after = moved(own, axis, 1), moved(own, axis, -1)
    upper, lower = moved(before[:half], axis, 1), moved(after[half:], axis, -1)
    return before, after, upper, lower


def one_hot_slots(block_routes, experts, capacity):
    tokens, top_count = block_routes.shape
    pairs = tokens * top_count
    named = block_routes.reshape(-1, 1) == jnp.arange(experts, dtype=jnp.int32)[None, :]
    named = named.astype(jnp.bfloat16)
    earlier = jnp.tril(jnp.ones((pairs, pairs), jnp.bfloat16), -1)
    before = jnp.dot(earlier, named, preferred_element_type=jnp.float32)
    ranking = jnp.sum(before * named.astype(jnp.float32), axis=1).astype(jnp.int32)
    return (block_routes.reshape(-1) * capacity + ranking).reshape(tokens, top_count)


def turned_rows(weights, steps, parts, me):
    height = weights.shape[0] // parts
    return jnp.concatenate(
        [
            lax.dynamic_slice_in_dim(weights, (me + step) % parts * height, height, axis=0)
            for step in steps
        ],
        axis=0,
    )


def added(sums, parts, steps, weights, gain):
    size, me = lax.axis_size("tp"), lax.axis_index("tp")
    rows = [part.astype(jnp.float32) for part in parts]
    square = sum(jnp.sum(part * part, axis=1, keepdims=True) for part in rows)
    scaled = jnp.concatenate(
        [
            (part * lax.dynamic_index_in_dim(gain, (me + step) % size, 0)).astype(jnp.bfloat16)
            for part, step in zip(rows, steps)
        ],
        axis=1,
    )
    gate, up = (jnp.dot(scaled, matrix, preferred_element_type=jnp.float32) for matrix in weights)
    if sums is None:
        return gate, up, square
    return sums[0] + gate, sums[1] + up, sums[2] + square


def ring_sum(own, right, left, far, axis):
    half = far.shape[0] // 2
    upper, lower = moved(far[:half], axis, 1), moved(far[half:], axis, -1)
    upper, lower = upper.astype(jnp.float32), lower.astype(jnp.float32)
    right_top = (right[:half].astype(jnp.float32) + upper).astype(jnp.bfloat16)
    left_low = (left[half:].astype(jnp.float32) + lower).astype(jnp.bfloat16)
    right = jnp.concatenate((right_top, right[half:]), axis=0)
    left = jnp.concatenate((left[:half], left_low), axis=0)
    from_left, from_right = moved(right, axis, 1), moved(left, axis, -1)
    arrived = from_left.astype(jnp.float32) + from_right.astype(jnp.float32)
    return own.astype(jnp.float32) + arrived


def layer(
    query_first,
    key_first,
    value_first,
    decay_first,
    gate_first,
    norm_first,
    proj_first,
    query_second,
    key_second,
    value_second,
    decay_second,
    gate_second,
    norm_second,
    proj_second,
    residual_in,
    expert_norm,
    route_ids,
    route_weight,
    expert_gate,
    expert_up,
    expert_down,
):
    bf16, f32 = jnp.bfloat16, jnp.float32
    tokens = query_first.shape[0]
    own_weights = jnp.concatenate((proj_first, proj_second), axis=0).T
    tp_size = lax.axis_size("tp")
    plane_size = lax.axis_size(SP[1]) * lax.axis_size(SP[2])
    planes = lax.axis_size(SP[0])
    sent = VA + VB + 128
    (states,) = call(
        state_kernel,
        [shaped((KA, sent), bf16)],
        key_first,
        value_first,
        decay_first,
        key_second,
        value_second,
        decay_second,
    )
    in_plane = lax.all_to_all(
        states.reshape(plane_size, KA // plane_size, sent), SP[1:], 0, 0, tiled=True
    )
    local_first, read_first, local_second, read_second = call(
        local_kernel,
        [shaped((tokens, n), f32) for n in (VA, KA, 2 * VB, 2 * KB)],
        query_first,
        key_first,
        value_first,
        decay_first,
        query_second,
        key_second,
        value_second,
        decay_second,
        flops=2_000_000_000,
    )
    copies = jnp.broadcast_to(own_weights[None], (planes, *own_weights.shape))
    columns = lax.all_to_all(copies, SP[0], split_axis=0, concat_axis=0, tiled=True)
    before, after, upper, lower = around(columns, SP[1])
    mine = jnp.concatenate((columns, before, after, upper, lower), axis=0)
    mine = mine.reshape(-1, *columns.shape)
    other = moved(mine, SP[2], 1)
    message, prefix, passed = call(
        plane_kernel,
        [
            shaped((planes, in_plane.shape[1], sent), bf16),
            shaped((*in_plane.shape[:2], VA + VB), f32),
            shaped((*in_plane.shape[:2], VA + VB), f32),
        ],
        in_plane,
        place=([lax.axis_index(SP[0])],),
    )
    told = lax.all_to_all(message, SP[0], split_axis=0, concat_axis=0, tiled=True)
    (entering,) = call(entering_kernel, [shaped(prefix.shape, bf16)], told, prefix, passed)
    carried = lax.all_to_all(entering, SP[1:], 0, 0, tiled=True).reshape(KA, VA + VB)
    tp_index = lax.axis_index("tp")
    (partial_terms,) = call(
        mix_kernel,
        [shaped((tp_size, tokens + residual_in.shape[0], residual_in.shape[1] // tp_size), bf16)],
        local_first,
        read_first,
        local_second,
        read_second,
        carried,
        gate_first,
        gate_second,
        norm_first.reshape(1, VA),
        norm_second.reshape(1, VB),
        mine,
        other,
        residual_in,
        place=([lax.axis_index(SP[1]), lax.axis_index(SP[2])],),
    )
    block_tokens, top_count = route_ids.shape
    experts = lax.axis_size(SP)
    capacity = 2 * top_count * block_tokens // experts
    arrived = lax.all_to_all(partial_terms, "tp", split_axis=0, concat_axis=0, tiled=True)
    mixture = arrived[:, :tokens].astype(jnp.float32).sum(axis=0)
    residual_part = arrived[:, tokens:].reshape(tokens, -1)
    residual = (residual_part.astype(jnp.float32) + mixture).astype(jnp.bfloat16)
    slots = one_hot_slots(route_ids, experts, capacity)
    width = residual.shape[1]
    model_width = width * tp_size
    share = capacity // CHUNKS
    rows_here = experts * share
    numbers = jnp.arange(rows_here, dtype=jnp.int32)
    waiting, shares = [], []
    for k in range(CHUNKS):
        held = numbers // share * capacity + k * share + numbers % share
        chosen = slots[:, :, None] == held[None, None, :]
        carries = jnp.any(chosen, axis=1).astype(bf16)
        shares.append(jnp.sum(jnp.where(chosen, route_weight[:, :, None], 0.0), axis=1))
        outgoing = lax.dot_general(
            carries, residual, (((0,), (0,)), ((), ())), preferred_element_type=f32
        ).astype(bf16)
        waiting.append(
            lax.all_to_all(outgoing.reshape(experts, share, width), SP, 0, 0, tiled=True)
        )
    gain = expert_norm.reshape(tp_size, width)
    turned, opposed = (
        tuple(
            turned_rows(matrix[0], steps, tp_size, tp_index)
            for matrix in (expert_gate, expert_up)
        )
        for steps in ((0, tp_size - 1, 1), (2,))
    )
    turned, opposed = lax.optimization_barrier((turned, opposed))
    returned = []
    for k in range(CHUNKS):
        incoming = waiting[k].reshape(rows_here, width)
        half = rows_here // 2
        top, low = moved(incoming[:half], "tp", 1), moved(incoming[half:], "tp", -1)
        next_low, next_top = moved(incoming[half:], "tp", 1), moved(incoming[:half], "tp", -1)
        upper, lower = moved(top, "tp", 1), moved(low, "tp", -1)
        before = jnp.concatenate((top, next_low), axis=0)
        after = jnp.concatenate((next_top, low), axis=0)
        far = jnp.concatenate((upper, lower), axis=0)
        sums = added(None, (incoming, before, after), (0, tp_size - 1, 1), turned, gain)
        sums = lax.optimization_barrier(sums)
        sums = added(sums, (far,), (2,), opposed, gain)
        scale = lax.rsqrt(sums[2] / model_width + epsilon)
        hidden = (jax.nn.silu(sums[0] * scale) * (sums[1] * scale)).astype(bf16)

        def produced(step, hidden=hidden):
            at = (tp_index + step) % tp_size * width
            down = lax.dynamic_slice_in_dim(expert_down[0], at, width, axis=1)
            return jnp.dot(hidden, down, preferred_element_type=f32).astype(bf16)

        opposite = produced(2)
        rest = lax.optimization_barrier((produced(0), produced(1), produced(tp_size - 1)))
        summed = ring_sum(*rest, opposite, "tp").astype(bf16)
        returned.append(lax.all_to_all(summed.reshape(experts, share, width), SP, 0, 0, tiled=True))
    combined = jnp.zeros((block_tokens, width), f32)
    for weights, back in zip(shares, returned):
        back = back.reshape(rows_here, width)
        coarse = lax.reduce_precision(weights, 8, 7)
        for portion in (coarse, weights - coarse):
            combined = combined + jnp.dot(portion.astype(bf16), back, preferred_element_type=f32)
    layer_part = (residual.astype(jnp.float32) + combined).astype(jnp.bfloat16)
    whole = lax.all_to_all(layer_part.reshape(tp_size, -1, width), "tp", 0, 0, tiled=True)
    return jnp.moveaxis(whole, 0, 1).reshape(block_tokens // tp_size, model_width)


def solution(mesh):
    split = Mesh(mesh.devices.reshape(8, 4, 2, mesh.shape["tp"]), ("sp_0", "sp_1", "sp_2", "tp"))
    in_specs = (
        P(SP, "tp"),
        P(SP, "tp"),
        P(SP, "tp"),
        P(SP, "tp"),
        P(SP, "tp"),
        P(),
        P("tp", SP),
        P(SP, "tp"),
        P(SP, "tp"),
        P(SP, "tp"),
        P(SP, "tp"),
        P(SP, "tp"),
        P(),
        P("tp", SP),
        P(SP_TP, None),
        P(),
        P(SP, None),
        P(SP, None),
        P(SP, None, "tp"),
        P(SP, None, "tp"),
        P(SP, "tp", None),
    )
    out_specs = P(SP_TP, None)
    return jax.shard_map(layer, mesh=split, in_specs=in_specs, out_specs=out_specs, check_vma=False)
```
